32 devices in a mesh: ep: 8 (over z, x), tp: 4 (over y, core).
Axes of the slice: x: 2, y: 2, z: 4, core: 2. Of those that a mesh axis runs over, the one named last changes fastest.
Arguments:
- residual: bfloat16 [512, 4096], P('ep', 'tp'), may hold values from -64 to 64
- routes: int32 [512, 2], P('ep'), may hold values from 0 to 7, all different within a row; in each aligned block of 64 rows (0 to 63, 64 to 127, ...) at most 32 rows name the same one
- route_weights: float32 [512, 2], P('ep'), may hold values from 0.2 to 1
- state_prev: float32 [512, 2, 64, 64], P('ep', None, 'tp'), may hold values from -6 to 6
- mix_gain: float32 [4096], replicated, may hold values from 0.1 to 1.9
- ffn_gain: float32 [4096], replicated, may hold values from 0.1 to 1.9
- w_in: bfloat16 [4096, 1024], P(None, 'tp'), may hold values from -0.09375 to 0.09375
- decay_rate: float32 [64, 64], P('tp'), may hold values from 0.5 to 8
- rotation: float32 [64, 64], P('tp'), may hold values from 0 to 200
- log_step: float32 [64], P('tp'), may hold values from -3.9 to -1.2
- in_re: float32 [64, 64, 16], P('tp'), may hold values from -1 to 1
- in_im: float32 [64, 64, 16], P('tp'), may hold values from -1 to 1
- read_re: float32 [64, 16, 64], P('tp'), may hold values from -0.5 to 0.5
- read_im: float32 [64, 16, 64], P('tp'), may hold values from -0.5 to 0.5
- skip_gain: float32 [64, 16], P('tp'), may hold values from -4 to 4
- w_glu: bfloat16 [1024, 1024], P(None, 'tp'), may hold values from -0.1875 to 0.1875
- w_out: bfloat16 [1024, 4096], P('tp'), may hold values from -0.1875 to 0.1875
- w_gate: bfloat16 [8, 4096, 5632], P('ep', None, 'tp'), may hold values from -0.09375 to 0.09375
- w_up: bfloat16 [8, 4096, 5632], P('ep', None, 'tp'), may hold values from -0.09375 to 0.09375
- w_down: bfloat16 [8, 5632, 4096], P('ep', 'tp'), may hold values from -0.078125 to 0.078125
Outputs:
- layer_out: bfloat16 [512, 4096], P('ep', 'tp')
- state_next: float32 [512, 2, 64, 64], P('ep', None, 'tp')
The draws below stay inside these ranges and needn't reach their ends.
Inputs may be any that keep to these rules, and one draw needn't show every extreme that they name: `routes`: each row names 2 different experts. In each aligned block of 64 rows (the rows of one index of ep) no expert is named more than 32 times, a bound that some block reaches.
All inputs are finite; a program needn't handle non-finite values.
Results may differ from the reference program's by a relative error of at most 0.012.
Values may be sent and summed in bfloat16 or wider, within the bound.
No kernel may reach another device: no remote copies, remote signals or barrier semaphores. Data moves between devices by JAX's collectives and lax.ppermute only.
A program may use at most 128 MiB of HBM per device.

```python
import math
import jax
import jax.numpy as jnp
import numpy as np
from jax import lax

D = 4096
CHAN = 1024
GROUP_CH = 16
GROUPS = 64
STATE = 64
FF_EXP = 5632
TOPK = 2
SEQ_GRP = 64
SEQS = 512
EXPERTS = 8
CAP = 32
N_EP = 8
N_TP = 4


def draw_residual(key, part):
    first_key, second_key = jax.random.split(jax.random.fold_in(key, 11))
    column_pos = jnp.arange(D, dtype=jnp.float32) / D
    row_scale = jnp.exp(math.log(10.0) * (jax.random.uniform(second_key, (SEQS, 1), jnp.float32) - 0.5))
    base_values = jnp.clip(jax.random.normal(first_key, (SEQS, D), jnp.float32), -6.0, 6.0)
    column_scale = jnp.exp(math.log(10.0) * (column_pos - 0.5))
    return (base_values * column_scale[None, :] * row_scale).astype(jnp.bfloat16)


def shard_levels(rng, dims, cuts, low, largest):
    def one(dim, shards_of):
        heights = jax.random.uniform(jax.random.fold_in(jax.random.fold_in(rng, 6), dim), (shards_of,), jnp.float32, low / len(cuts), largest / len(cuts))
        return jnp.repeat(jnp.exp(heights), dims[dim] // shards_of).reshape((-1,) + (1,) * (len(dims) - dim - 1))

    factor_of = one(*cuts[0])
    for cut in cuts[1:]:
        factor_of = factor_of * one(*cut)
    return factor_of


def deal_out(own_key, own, number, rows, number_of, top, limit, lean):
    sequence = jax.random.permutation(own_key, number_of)
    packed, usual = portions_of(number_of, rows * top, limit, lean, True), portions_of(number_of, rows * top, limit, lean, False)
    places = jnp.arange(number_of)

    def named(sizes, turn):
        used = int((sizes > 0).sum())
        fixed = max(1, used // 4)
        moved = fixed + (places - fixed + turn * (used - fixed)) % max(1, number_of - fixed)
        return jnp.zeros((number_of,), jnp.int32).at[sequence[jnp.where(places < fixed, places, moved)]].set(jnp.asarray(sizes, jnp.int32))

    sizes = jnp.where(number % 4 == 0, named(packed, number // 4), named(usual, number - number // 4 - 1))
    mixed = jax.random.permutation(jax.random.fold_in(own, 3), number_of)
    giver, taker = mixed[0:number_of // 2 * 2:2], mixed[1:number_of // 2 * 2:2]
    room = jnp.minimum(sizes[giver] - 1, limit - sizes[taker]) // 2
    room = jnp.where((giver == sequence[0]) | (taker == sequence[0]) | (sizes[taker] == 0), 0, jnp.maximum(room, 0))
    moved = jax.random.randint(jax.random.fold_in(own, 4), (number_of // 2,), 0, 1 << 20) % (room + 1)
    sizes = sizes.at[giver].add(-moved).at[taker].add(moved)
    items = jnp.searchsorted(jnp.cumsum(sizes), jnp.arange(rows * top), side="right").astype(jnp.int32)
    listing = items.reshape(top, rows).T
    listing = listing[jax.random.permutation(jax.random.fold_in(own, 1), rows)]
    turn = jax.random.randint(jax.random.fold_in(own, 2), (rows, 1), 0, top)
    return jnp.take_along_axis(listing, (jnp.arange(top)[None, :] + turn) % top, axis=1)


def portions_of(amount, total, reach, lean, full):
    portions = [(1 << 20) // math.isqrt(rank ** lean) + 1 for rank in range(1, amount + 1)]
    largest = reach if full else min(reach, max(-(-total // amount), total * portions[0] // sum(portions)))
    least = 1 if total - largest >= amount - 1 else 0
    holding, surplus = [largest] + [least] * (amount - 1), total - largest - least * (amount - 1)
    while surplus > 0:
        movable = [i for i in range(1, amount) if holding[i] < largest] or [i for i in range(1, amount) if holding[i] < reach]
        mass, left = sum([portions[i] for i in movable]), surplus
        for i in movable:
            addition = min(reach - holding[i], max(1, left * portions[i] // mass), surplus)
            holding[i] = holding[i] + addition
            surplus = surplus - addition
    return np.array(holding)


def noise(rng, dims, deviation, bound, shards=(), held_as=jnp.bfloat16):
    factor_of = shard_levels(rng, dims, shards, -0.22, 0.18) if shards else 1.0
    array = jax.random.normal(rng, dims, jnp.float32) * deviation * factor_of
    return jnp.minimum(jnp.maximum(array, -bound), bound).astype(held_as)


def setup_inputs(seed: int = 0) -> dict:
    keys = jax.random.split(jax.random.key(seed), 21)
    residual = draw_residual(jax.random.fold_in(keys[20], 71), 0)
    routes_keys = jax.random.split(jax.random.fold_in(keys[1], 1), SEQS // SEQ_GRP)
    routes_turns = jax.random.permutation(jax.random.fold_in(keys[1], 3), SEQS // SEQ_GRP)
    routes = jax.vmap(lambda own, number: deal_out(jax.random.fold_in(keys[1], 2), own, number, SEQ_GRP, EXPERTS, TOPK, CAP, 1))(routes_keys, routes_turns).reshape((SEQS, TOPK))
    route_weights = jnp.clip(0.2 + 0.8 * jax.random.uniform(keys[2], (SEQS, TOPK), jnp.float32) ** shard_levels(keys[2], (SEQS, TOPK), ((0, 8),), -0.2, 0.2), 0.2, 1.0)
    state_prev = noise(keys[3], (SEQS, 2, GROUPS, STATE), 1.0, 6.0, ((0, 8), (2, 4)), jnp.float32)
    mix_gain = jnp.clip(1.0 + 0.18 * jax.random.normal(keys[4], (D,), jnp.float32), 0.1, 1.9)
    ffn_gain = jnp.clip(1.0 + 0.18 * jax.random.normal(keys[5], (D,), jnp.float32), 0.1, 1.9)
    w_in = noise(keys[6], (D, CHAN), D ** -0.5, 0.09375, ((1, 4),))
    decay_rate = jnp.clip(jnp.exp(math.log(8.0) - 2.7725887 * jax.random.uniform(keys[7], (GROUPS, STATE), jnp.float32) ** shard_levels(keys[7], (GROUPS, STATE), ((0, 4),), -0.2, 0.2)), 0.5, 8.0)
    rotation = jnp.clip(200.0 * jax.random.uniform(keys[8], (GROUPS, STATE), jnp.float32) ** shard_levels(keys[8], (GROUPS, STATE), ((0, 4),), -0.2, 0.2), 0.0, 200.0)
    log_step = jnp.clip(-3.9 + 2.7 * jax.random.uniform(keys[9], (GROUPS,), jnp.float32) ** shard_levels(keys[9], (GROUPS,), ((0, 4),), -0.2, 0.2), -3.9, -1.2)
    in_re = noise(keys[10], (GROUPS, STATE, GROUP_CH), (2 * GROUP_CH) ** -0.5, 1.0, ((0, 4),), jnp.float32)
    in_im = noise(keys[11], (GROUPS, STATE, GROUP_CH), (2 * GROUP_CH) ** -0.5, 1.0, ((0, 4),), jnp.float32)
    read_re = noise(keys[12], (GROUPS, GROUP_CH, STATE), (2 * STATE) ** -0.5, 0.5, ((0, 4),), jnp.float32)
    read_im = noise(keys[13], (GROUPS, GROUP_CH, STATE), (2 * STATE) ** -0.5, 0.5, ((0, 4),), jnp.float32)
    skip_gain = noise(keys[14], (GROUPS, GROUP_CH), 1.0, 4.0, ((0, 4),), jnp.float32)
    w_glu = noise(keys[15], (CHAN, CHAN), CHAN ** -0.5, 0.1875, ((1, 4),))
    w_out = noise(keys[16], (CHAN, D), CHAN ** -0.5, 0.1875, ((0, 4),))
    w_gate = noise(keys[17], (EXPERTS, D, FF_EXP), D ** -0.5, 0.09375, ((0, 8), (2, 4)))
    w_up = noise(keys[18], (EXPERTS, D, FF_EXP), D ** -0.5, 0.09375, ((0, 8), (2, 4)))
    w_down = noise(keys[19], (EXPERTS, FF_EXP, D), FF_EXP ** -0.5, 0.078125, ((0, 8), (1, 4)))
    return dict(residual=residual, routes=routes, route_weights=route_weights, state_prev=state_prev, mix_gain=mix_gain, ffn_gain=ffn_gain, w_in=w_in, decay_rate=decay_rate, rotation=rotation, log_step=log_step, in_re=in_re, in_im=in_im, read_re=read_re, read_im=read_im, skip_gain=skip_gain, w_glu=w_glu, w_out=w_out, w_gate=w_gate, w_up=w_up, w_down=w_down)


epsilon = 1e-06
highest = lax.Precision.HIGHEST

def inverse_rms(values):
    return lax.rsqrt(lax.optimization_barrier(jnp.mean(values * values, axis=-1, keepdims=True)) + epsilon)

def state_mixer(u_in, state_prev, decay_rate, rotation, log_step, in_re, in_im, read_re, read_im, skip_gain):
    batch_rows = u_in.shape[0]
    groups = decay_rate.shape[0]
    grouped = u_in.astype(jnp.float32).reshape(batch_rows, groups, GROUP_CH)
    step_size = jnp.exp(log_step)[:, None]
    real_part = -decay_rate
    magnitude = jnp.exp(real_part * step_size)
    decay_re = magnitude * jnp.cos(rotation * step_size)
    decay_im = magnitude * jnp.sin(rotation * step_size)
    denominator = real_part * real_part + rotation * rotation
    lift_re = ((decay_re - 1.0) * real_part + decay_im * rotation) / denominator
    lift_im = (decay_im * real_part - (decay_re - 1.0) * rotation) / denominator
    map_re = lift_re[..., None] * in_re - lift_im[..., None] * in_im
    map_im = lift_re[..., None] * in_im + lift_im[..., None] * in_re
    drive_re = jnp.einsum('gph,bgh->bgp', map_re, grouped, precision=highest)
    drive_im = jnp.einsum('gph,bgh->bgp', map_im, grouped, precision=highest)
    old_re = state_prev[:, 0]
    old_im = state_prev[:, 1]
    new_re = decay_re * old_re - decay_im * old_im + drive_re
    new_im = decay_re * old_im + decay_im * old_re + drive_im
    output = jnp.einsum('ghp,bgp->bgh', read_re, new_re, precision=highest) - jnp.einsum('ghp,bgp->bgh', read_im, new_im, precision=highest) + skip_gain * grouped
    return (jax.nn.gelu(output.reshape(batch_rows, -1)), jnp.stack([new_re, new_im], axis=1))

def reference(residual, routes, route_weights, state_prev, mix_gain, ffn_gain, w_in, decay_rate, rotation, log_step, in_re, in_im, read_re, read_im, skip_gain, w_glu, w_out, w_gate, w_up, w_down):
    source = residual.astype(jnp.float32)
    normed_mix = (source * inverse_rms(source) * mix_gain).astype(jnp.bfloat16)
    u_in = jnp.dot(normed_mix, w_in, preferred_element_type=jnp.float32).astype(jnp.bfloat16)
    mixer_act, state_next = state_mixer(u_in, state_prev, decay_rate, rotation, log_step, in_re, in_im, read_re, read_im, skip_gain)
    mixer_bf = mixer_act.astype(jnp.bfloat16)
    glu_logit = jnp.dot(mixer_bf, w_glu, preferred_element_type=jnp.float32)
    mixed = (mixer_act * jax.nn.sigmoid(glu_logit)).astype(jnp.bfloat16)
    block_width = CHAN // N_TP
    branch = jnp.zeros((SEQS, D), jnp.float32)
    for shard in range(N_TP):
        partial_block = jnp.dot(mixed[:, shard * block_width:(shard + 1) * block_width], w_out[shard * block_width:(shard + 1) * block_width], preferred_element_type=jnp.float32).astype(jnp.bfloat16)
        branch = branch + lax.optimization_barrier(partial_block).astype(jnp.float32)
    after_mix = (source + branch).astype(jnp.bfloat16)
    after_float = after_mix.astype(jnp.float32)
    normed_ffn = (after_float * inverse_rms(after_float) * ffn_gain).astype(jnp.bfloat16)
    expert_ids = jnp.arange(EXPERTS, dtype=jnp.int32)
    onehot = (routes[:, :, None] == expert_ids).astype(jnp.int32)
    blocked = onehot.reshape(N_EP, SEQ_GRP * TOPK, EXPERTS)
    before = jnp.cumsum(blocked, axis=1) - blocked
    slot_index = lax.optimization_barrier(jnp.sum(before * blocked, axis=-1)).reshape(SEQS, TOPK)
    group_of_row = jnp.arange(SEQS, dtype=jnp.int32) // SEQ_GRP
    position = group_of_row[:, None] * CAP + slot_index
    columns = jnp.arange(N_EP * CAP, dtype=jnp.int32)
    hidden_width = FF_EXP // N_TP
    normed_float = normed_ffn.astype(jnp.float32)

    def apply_expert(running, expert):
        matches = (routes == expert)[:, :, None] & (position[:, :, None] == columns)
        select = jnp.any(matches, axis=1).astype(jnp.float32)
        weighting = lax.optimization_barrier(jnp.sum(jnp.where(matches, route_weights[:, :, None], 0.0), axis=1))
        expert_in = jnp.dot(select.T, normed_float, precision=highest).astype(jnp.bfloat16)
        gate_value = jnp.dot(expert_in, w_gate[expert], preferred_element_type=jnp.float32)
        up_value = jnp.dot(expert_in, w_up[expert], preferred_element_type=jnp.float32)
        hidden = (jax.nn.silu(gate_value) * up_value).astype(jnp.bfloat16)
        down_weight = w_down[expert]
        summed = jnp.zeros((N_EP * CAP, D), jnp.float32)
        for shard in range(N_TP):
            partial_block = jnp.dot(hidden[:, shard * hidden_width:(shard + 1) * hidden_width], down_weight[shard * hidden_width:(shard + 1) * hidden_width], preferred_element_type=jnp.float32).astype(jnp.bfloat16)
            summed = summed + lax.optimization_barrier(partial_block).astype(jnp.float32)
        expert_out = summed.astype(jnp.bfloat16)
        added = jnp.dot(weighting, expert_out.astype(jnp.float32), precision=highest)
        return (running + added, None)
    combined, _ = lax.scan(apply_expert, jnp.zeros((SEQS, D), jnp.float32), expert_ids)
    layer_out = (after_float + combined).astype(jnp.bfloat16)
    return (layer_out, state_next)
```

```python
import jax
import jax.numpy as jnp
from jax import lax
from jax.sharding import PartitionSpec as P

GROUP_CH = 16
TOPK = 2


epsilon = 1e-06
highest = lax.Precision.HIGHEST


def state_mixer(
    u_in, state_prev, decay_rate, rotation, log_step, in_re, in_im, read_re, read_im, skip_gain
):
    batch_rows = u_in.shape[0]
    groups = decay_rate.shape[0]
    grouped = u_in.astype(jnp.float32).reshape(batch_rows, groups, GROUP_CH)
    step_size = jnp.exp(log_step)[:, None]
    real_part = -decay_rate
    magnitude = jnp.exp(real_part * step_size)
    decay_re = magnitude * jnp.cos(rotation * step_size)
    decay_im = magnitude * jnp.sin(rotation * step_size)
    denominator = real_part * real_part + rotation * rotation
    lift_re = ((decay_re - 1.0) * real_part + decay_im * rotation) / denominator
    lift_im = (decay_im * real_part - (decay_re - 1.0) * rotation) / denominator
    map_re = lift_re[..., None] * in_re - lift_im[..., None] * in_im
    map_im = lift_re[..., None] * in_im + lift_im[..., None] * in_re
    drive_re = jnp.einsum("gph,bgh->bgp", map_re, grouped, precision=highest)
    drive_im = jnp.einsum("gph,bgh->bgp", map_im, grouped, precision=highest)
    old_re = state_prev[:, 0]
    old_im = state_prev[:, 1]
    new_re = decay_re * old_re - decay_im * old_im + drive_re
    new_im = decay_re * old_im + decay_im * old_re + drive_im
    output = (
        jnp.einsum("ghp,bgp->bgh", read_re, new_re, precision=highest)
        - jnp.einsum("ghp,bgp->bgh", read_im, new_im, precision=highest)
        + skip_gain * grouped
    )
    return (jax.nn.gelu(output.reshape(batch_rows, -1)), jnp.stack([new_re, new_im], axis=1))


def per_device(
    residual,
    routes,
    route_weights,
    state_prev,
    mix_gain,
    ffn_gain,
    w_in,
    decay_rate,
    rotation,
    log_step,
    in_re,
    in_im,
    read_re,
    read_im,
    skip_gain,
    w_glu,
    w_out,
    w_gate,
    w_up,
    w_down,
):
    width = residual.shape[1]
    rows = residual.shape[0]
    tp_size = lax.axis_size("tp")
    ep_size = lax.axis_size("ep")
    chips = tp_size // 2
    full_width = width * tp_size
    place = lax.axis_index("tp")
    core = place % 2
    chip = place // 2
    expert_here = lax.axis_index("ep")
    capacity = 2 * rows * TOPK // ep_size
    f32 = jnp.float32
    bf16 = jnp.bfloat16

    def swap_core(value):
        return lax.ppermute(value, "tp", [(i, i ^ 1) for i in range(tp_size)])

    def swap_chip(value, step):
        return lax.ppermute(value, "tp", [(i, i ^ (2 * step)) for i in range(tp_size)])

    def swap_expert(value, step):
        return lax.ppermute(value, "ep", [(i, i ^ step) for i in range(ep_size)])

    def spot(step, same_core):
        return 2 * (chip ^ step) + (core if same_core else 1 - core)

    def reduce_over_tp(partial_for):
        away = []
        for step in range(1, chips):
            theirs = swap_core(partial_for(spot(step, False)).astype(bf16))
            ours = partial_for(spot(step, True))
            away.append(swap_chip((ours + theirs.astype(f32)).astype(bf16), step))
        theirs = swap_core(partial_for(spot(0, False)).astype(bf16))
        total = partial_for(spot(0, True)) + theirs.astype(f32)
        for piece in away:
            total = total + piece.astype(f32)
        return total

    flat_routes = routes.reshape(-1)
    onehot = (flat_routes[:, None] == jnp.arange(ep_size, dtype=jnp.int32)).astype(jnp.int32)
    before = jnp.cumsum(onehot, axis=0) - onehot
    slot_index = jnp.sum(before * onehot, axis=1)
    relative = jnp.bitwise_xor(flat_routes, expert_here)
    destination = (relative * capacity + slot_index).reshape(rows, TOPK)
    matches = destination[:, :, None] == jnp.arange(ep_size * capacity, dtype=jnp.int32)
    dispatch_map = jnp.any(matches, axis=1).astype(bf16)

    gathered = lax.all_gather(residual, "tp", axis=1, tiled=True).astype(f32)
    squares = jnp.mean(gathered * gathered, axis=1, keepdims=True)
    normed_mix = (gathered * lax.rsqrt(squares + epsilon) * mix_gain).astype(bf16)
    u_in = jnp.dot(normed_mix, w_in, preferred_element_type=f32).astype(bf16)
    mixer_act, state_next = state_mixer(
        u_in, state_prev, decay_rate, rotation, log_step, in_re, in_im, read_re, read_im, skip_gain
    )
    all_channels = lax.all_gather(mixer_act.astype(bf16), "tp", axis=1, tiled=True)
    glu_logit = jnp.dot(all_channels, w_glu, preferred_element_type=f32)
    mixed = (mixer_act * jax.nn.sigmoid(glu_logit)).astype(bf16)
    partial_out = jnp.dot(mixed, w_out, preferred_element_type=f32)
    branch = reduce_over_tp(
        lambda spot_of: lax.dynamic_slice_in_dim(partial_out, spot_of * width, width, 1)
    )
    after_mix = (residual.astype(f32) + branch).astype(bf16)

    outbound = lax.dot_general(
        dispatch_map, after_mix, (((0,), (0,)), ((), ())), preferred_element_type=f32
    ).astype(bf16)
    blocks = [outbound[k * capacity : (k + 1) * capacity] for k in range(ep_size)]
    arrived = jnp.concatenate(
        [blocks[0]] + [swap_expert(blocks[k], k) for k in range(1, ep_size)], axis=0
    )
    pieces = [(spot(0, True), arrived)]
    partner = swap_core(arrived)
    far = [swap_chip(arrived, step) for step in range(1, chips)]
    pieces.append((spot(0, False), partner))
    for step in range(1, chips):
        pieces.append((spot(step, True), far[step - 1]))
    for step in range(1, chips):
        pieces.append((spot(step, False), swap_core(far[step - 1])))
    gate_value = up_value = total_squares = 0.0
    for spot_of, piece in pieces:
        wide = piece.astype(f32)
        total_squares = total_squares + jnp.sum(wide * wide, axis=1, keepdims=True)
        gain_here = lax.dynamic_slice_in_dim(ffn_gain, spot_of * width, width)
        gained = (wide * gain_here).astype(bf16)
        gate_here = lax.dynamic_slice_in_dim(w_gate[0], spot_of * width, width, 0)
        up_here = lax.dynamic_slice_in_dim(w_up[0], spot_of * width, width, 0)
        gate_value = gate_value + jnp.dot(gained, gate_here, preferred_element_type=f32)
        up_value = up_value + jnp.dot(gained, up_here, preferred_element_type=f32)
    scale_rows = lax.rsqrt(total_squares / full_width + epsilon)
    hidden = (jax.nn.silu(gate_value * scale_rows) * (up_value * scale_rows)).astype(bf16)

    def down_for(spot_of):
        part = lax.dynamic_slice_in_dim(w_down[0], spot_of * width, width, 1)
        return jnp.dot(hidden, part, preferred_element_type=f32)

    reduced = reduce_over_tp(down_for).astype(bf16)
    blocks = [reduced[k * capacity : (k + 1) * capacity] for k in range(ep_size)]
    came_back = jnp.concatenate(
        [blocks[0]] + [swap_expert(blocks[k], k) for k in range(1, ep_size)], axis=0
    )
    combined = 0.0
    for k in range(TOPK):
        picked = jnp.dot(matches[:, k].astype(bf16), came_back, preferred_element_type=f32)
        combined = combined + route_weights[:, k : k + 1] * picked
    layer_out = (after_mix.astype(f32) + combined).astype(bf16)
    return (layer_out, state_next)


def solution(mesh):
    return jax.shard_map(
        per_device,
        mesh=mesh,
        in_specs=(
            P("ep", "tp"),
            P("ep", None),
            P("ep", None),
            P("ep", None, "tp", None),
            P(),
            P(),
            P(None, "tp"),
            P("tp", None),
            P("tp", None),
            P("tp"),
            P("tp", None, None),
            P("tp", None, None),
            P("tp", None, None),
            P("tp", None, None),
            P("tp", None),
            P(None, "tp"),
            P("tp", None),
            P("ep", None, "tp"),
            P("ep", None, "tp"),
            P("ep", "tp", None),
        ),
        out_specs=(P("ep", "tp"), P("ep", None, "tp", None)),
        check_vma=False,
    )
```

```python
import functools

import jax
import jax.numpy as jnp
from jax import lax
from jax.experimental import pallas as pl
from jax.experimental.pallas import tpu as pltpu
from jax.sharding import PartitionSpec as P

GROUP_CH = 16
TOPK = 2


epsilon = 1e-06
highest = lax.Precision.HIGHEST


def state_mixer(
    u_in, state_prev, decay_rate, rotation, log_step, in_re, in_im, read_re, read_im, skip_gain
):
    batch_rows = u_in.shape[0]
    groups = decay_rate.shape[0]
    grouped = u_in.astype(jnp.float32).reshape(batch_rows, groups, GROUP_CH)
    step_size = jnp.exp(log_step)[:, None]
    real_part = -decay_rate
    magnitude = jnp.exp(real_part * step_size)
    decay_re = magnitude * jnp.cos(rotation * step_size)
    decay_im = magnitude * jnp.sin(rotation * step_size)
    denominator = real_part * real_part + rotation * rotation
    lift_re = ((decay_re - 1.0) * real_part + decay_im * rotation) / denominator
    lift_im = (decay_im * real_part - (decay_re - 1.0) * rotation) / denominator
    map_re = lift_re[..., None] * in_re - lift_im[..., None] * in_im
    map_im = lift_re[..., None] * in_im + lift_im[..., None] * in_re
    drive_re = jnp.einsum("gph,bgh->bgp", map_re, grouped, precision=highest)
    drive_im = jnp.einsum("gph,bgh->bgp", map_im, grouped, precision=highest)
    old_re = state_prev[:, 0]
    old_im = state_prev[:, 1]
    new_re = decay_re * old_re - decay_im * old_im + drive_re
    new_im = decay_re * old_im + decay_im * old_re + drive_im
    output = (
        jnp.einsum("ghp,bgp->bgh", read_re, new_re, precision=highest)
        - jnp.einsum("ghp,bgp->bgh", read_im, new_im, precision=highest)
        + skip_gain * grouped
    )
    return (jax.nn.gelu(output.reshape(batch_rows, -1)), jnp.stack([new_re, new_im], axis=1))


def products_kernel(counts, full_width, first, last, *refs):
    refs = list(refs)
    spots = refs.pop(0)
    gains = refs.pop(0)
    pieces = [[refs.pop(0) for _ in range(n)] for n in counts]
    before = None if first else [refs.pop(0) for _ in range(3)]
    w_gate, w_up = refs.pop(0), refs.pop(0)
    outs = [refs.pop(0)] if last else [refs.pop(0) for _ in range(3)]
    gate_buf, up_buf, scaled, sems = refs[:4]
    gate_acc, up_acc = refs[4:] if last else outs[:2]
    width = scaled.shape[1]
    depth = gate_buf.shape[1]
    steps = [(i, j) for i in range(len(counts)) for j in range(width // depth)]
    copies = []
    for n, (i, j) in enumerate(steps):
        start = pl.multiple_of(spots[i] * width + j * depth, depth)
        for m, (weights, buf) in enumerate(((w_gate, gate_buf), (w_up, up_buf))):
            copy = pltpu.make_async_copy(weights.at[0, pl.ds(start, depth)], buf.at[n], sems.at[m, n])
            copy.start()
            copies.append(copy)
    squares = 0.0 if first else before[2][...]
    started = not first
    if started and last:
        gate_acc[...] = before[0][...]
        up_acc[...] = before[1][...]
    for n, (i, j) in enumerate(steps):
        if j == 0:
            gain = gains[pl.ds(spots[i], 1), :]
            parts = []
            at = 0
            for group in pieces[i]:
                wide = group[...].astype(jnp.float32)
                parts.append(jnp.sum(wide * wide, axis=1, keepdims=True))
                scaled[at : at + group.shape[0], :] = (wide * gain).astype(jnp.bfloat16)
                at += group.shape[0]
            squares = squares + jnp.concatenate(parts, axis=0)
        left = scaled[:, j * depth : (j + 1) * depth]
        for m, (buf, acc) in enumerate(((gate_buf, gate_acc), (up_buf, up_acc))):
            copies[2 * n + m].wait()
            product = jnp.dot(left, buf[n], preferred_element_type=jnp.float32)
            if n > 0 or (started and last):
                acc[...] += product
            elif started:
                acc[...] = before[m][...] + product
            else:
                acc[...] = product
    if last:
        scale = lax.rsqrt(squares / full_width + epsilon)
        outs[0][...] = (jax.nn.silu(gate_acc[...] * scale) * (up_acc[...] * scale)).astype(jnp.bfloat16)
    else:
        outs[2][...] = squares


def expert_products(spots, gains, pieces, before, w_gate, w_up, full_width, last):
    counts = tuple(len(groups) for groups in pieces)
    width = gains.shape[1]
    rows = sum(group.shape[0] for group in pieces[0])
    units = w_gate.shape[2]
    depth = min(width, 512)
    steps = len(pieces) * (width // depth)
    first = before is None
    grid_free = pl.BlockSpec(memory_space=pltpu.VMEM)
    inputs = [gains, *(group for groups in pieces for group in groups), *(() if first else before)]
    acc = jax.ShapeDtypeStruct((rows, units), jnp.float32)
    if last:
        out_shape = [jax.ShapeDtypeStruct((rows, units), jnp.bfloat16)]
    else:
        out_shape = [acc, acc, jax.ShapeDtypeStruct((rows, 1), jnp.float32)]
    scratch = [
        pltpu.VMEM((steps, depth, units), jnp.bfloat16),
        pltpu.VMEM((steps, depth, units), jnp.bfloat16),
        pltpu.VMEM((rows, width), jnp.bfloat16),
        pltpu.SemaphoreType.DMA((2, steps)),
    ]
    if last:
        scratch += [pltpu.VMEM((rows, units), jnp.float32)] * 2
    return pl.pallas_call(
        functools.partial(products_kernel, counts, full_width, first, last),
        out_shape=out_shape,
        in_specs=[pl.BlockSpec(memory_space=pltpu.SMEM)]
        + [grid_free] * len(inputs)
        + [pl.BlockSpec(memory_space=pl.ANY)] * 2,
        out_specs=[grid_free] * len(out_shape),
        scratch_shapes=scratch,
        compiler_params=pltpu.CompilerParams(vmem_limit_bytes=40 * 2**20),
        cost_estimate=pl.CostEstimate(
            flops=4 * rows * width * units * len(pieces),
            bytes_accessed=4 * width * units * len(pieces),
            transcendentals=0,
        ),
    )(spots, *inputs, w_gate, w_up)


def per_device(
    residual,
    routes,
    route_weights,
    state_prev,
    mix_gain,
    ffn_gain,
    w_in,
    decay_rate,
    rotation,
    log_step,
    in_re,
    in_im,
    read_re,
    read_im,
    skip_gain,
    w_glu,
    w_out,
    w_gate,
    w_up,
    w_down,
):
    width = residual.shape[1]
    rows = residual.shape[0]
    tp_size = lax.axis_size("tp")
    ep_size = lax.axis_size("ep")
    chips = tp_size // 2
    full_width = width * tp_size
    place = lax.axis_index("tp")
    core = lax.bitwise_and(place, 1)
    chip = lax.shift_right_logical(place, 1)
    expert_here = lax.axis_index("ep")
    capacity = 2 * rows * TOPK // ep_size
    halves = ((0, ep_size // 2), (ep_size // 2, ep_size))
    f32 = jnp.float32
    bf16 = jnp.bfloat16

    def swap_core(value, label):
        with jax.named_scope(label):
            return lax.ppermute(value, "tp", [(i, i ^ 1) for i in range(tp_size)])

    def swap_chip(value, step, label):
        with jax.named_scope(label):
            return lax.ppermute(value, "tp", [(i, i ^ (2 * step)) for i in range(tp_size)])

    def swap_expert(value, step, label):
        with jax.named_scope(label + str(step)):
            return lax.ppermute(value, "ep", [(i, i ^ step) for i in range(ep_size)])

    def spot(step, same_core):
        return 2 * (chip ^ step) + (core if same_core else 1 - core)

    flat_routes = routes.reshape(-1)
    onehot = (flat_routes[:, None] == jnp.arange(ep_size, dtype=jnp.int32)).astype(jnp.int32)
    before = jnp.cumsum(onehot, axis=0) - onehot
    slot_index = jnp.sum(before * onehot, axis=1)
    relative = jnp.bitwise_xor(flat_routes, expert_here)
    destination = (relative * capacity + slot_index).reshape(rows, TOPK)
    matches = destination[:, :, None] == jnp.arange(ep_size * capacity, dtype=jnp.int32)
    dispatch_map = jnp.any(matches, axis=1).astype(bf16)
    gains = ffn_gain.reshape(tp_size, width)

    gathered = lax.all_gather(residual, "tp", axis=1, tiled=True).astype(f32)
    squares = jnp.mean(gathered * gathered, axis=1, keepdims=True)
    normed_mix = (gathered * lax.rsqrt(squares + epsilon) * mix_gain).astype(bf16)
    u_in = jnp.dot(normed_mix, w_in, preferred_element_type=f32).astype(bf16)
    mixer_act, state_next = state_mixer(
        u_in, state_prev, decay_rate, rotation, log_step, in_re, in_im, read_re, read_im, skip_gain
    )
    all_channels = lax.all_gather(mixer_act.astype(bf16), "tp", axis=1, tiled=True)
    glu_logit = jnp.dot(all_channels, w_glu, preferred_element_type=f32)
    mixed = lax.optimization_barrier((mixer_act * jax.nn.sigmoid(glu_logit)).astype(bf16))

    def branch_for(spot_of):
        part = lax.dynamic_slice_in_dim(w_out, spot_of * width, width, 1)
        return jnp.dot(mixed, part, preferred_element_type=f32)

    away = []
    for step in range(1, chips):
        theirs = swap_core(branch_for(spot(step, False)).astype(bf16), "branch_core")
        ours = branch_for(spot(step, True))
        away.append(swap_chip((ours + theirs.astype(f32)).astype(bf16), step, "branch_chip"))
    theirs = swap_core(branch_for(spot(0, False)).astype(bf16), "branch_home")
    branch = branch_for(spot(0, True)) + theirs.astype(f32)
    for piece in away:
        branch = branch + piece.astype(f32)
    after_mix = (residual.astype(f32) + branch).astype(bf16)

    outbound = lax.dot_general(
        dispatch_map, after_mix, (((0,), (0,)), ((), ())), preferred_element_type=f32
    ).astype(bf16)
    near_far = []
    for low, high in halves:
        blocks = [
            swap_expert(outbound[k * capacity : (k + 1) * capacity], k, "out")
            if k
            else outbound[:capacity]
            for k in range(low, high)
        ]
        near_far.append(jnp.concatenate(blocks, axis=0))
    own = [(spot(0, True), near_far), (spot(0, False), [swap_core(h, "gather_core") for h in near_far])]
    away = [[swap_chip(h, step, "gather_chip") for h in near_far] for step in range(1, chips)]
    same = [(spot(step, True), away[step - 1]) for step in range(1, chips)]
    cross = [
        (spot(step, False), [swap_core(h, "gather_cross") for h in away[step - 1]])
        for step in range(1, chips)
    ]
    sums = None
    for pieces, last, label in ((own, False, "own"), (same, False, "same"), (cross, True, "cross")):
        with jax.named_scope(label):
            spots = jnp.stack([p[0] for p in pieces]).astype(jnp.int32)
            sums = expert_products(
                spots, gains, [p[1] for p in pieces], sums, w_gate, w_up, full_width, last
            )
    hidden = sums[0]

    def down_for(spot_of):
        part = lax.dynamic_slice_in_dim(w_down[0], spot_of * width, width, 1)
        return jnp.dot(hidden, part, preferred_element_type=f32)

    spans = [slice(low * capacity, high * capacity) for low, high in halves]
    away = []
    for step in range(1, chips):
        theirs = swap_core(down_for(spot(step, False)).astype(bf16), "down_core")
        ours = (down_for(spot(step, True)) + theirs.astype(f32)).astype(bf16)
        away.append([swap_chip(ours[s], step, "down_chip" + str(i)) for i, s in enumerate(spans)])
    theirs = swap_core(down_for(spot(0, False)).astype(bf16), "down_home")
    home = down_for(spot(0, True)) + theirs.astype(f32)
    blocks = [None] * ep_size
    for i in (1, 0):
        total = home[spans[i]]
        for piece in away:
            total = total + piece[i].astype(f32)
        total = total.astype(bf16)
        for n, k in enumerate(range(*halves[i])):
            block = total[n * capacity : (n + 1) * capacity]
            blocks[k] = swap_expert(block, k, "back") if k else block
    came_back = jnp.concatenate(blocks, axis=0)
    combined = 0.0
    for k in range(TOPK):
        picked = jnp.dot(matches[:, k].astype(bf16), came_back, preferred_element_type=f32)
        combined = combined + route_weights[:, k : k + 1] * picked
    layer_out = (after_mix.astype(f32) + combined).astype(bf16)
    return (layer_out, state_next)


def solution(mesh):
    return jax.shard_map(
        per_device,
        mesh=mesh,
        in_specs=(
            P("ep", "tp"),
            P("ep", None),
            P("ep", None),
            P("ep", None, "tp", None),
            P(),
            P(),
            P(None, "tp"),
            P("tp", None),
            P("tp", None),
            P("tp"),
            P("tp", None, None),
            P("tp", None, None),
            P("tp", None, None),
            P("tp", None, None),
            P("tp", None),
            P(None, "tp"),
            P("tp", None),
            P("ep", None, "tp"),
            P("ep", None, "tp"),
            P("ep", "tp", None),
        ),
        out_specs=(P("ep", "tp"), P("ep", None, "tp", None)),
        check_vma=False,
    )
```

```python
import functools

import jax
import jax.numpy as jnp
from jax import lax
from jax.experimental import pallas as pl
from jax.experimental.pallas import tpu as pltpu
from jax.sharding import PartitionSpec as P


GROUP_CH = 16
TOPK = 2


epsilon = 1e-06
highest = lax.Precision.HIGHEST


def state_mixer(
    u_in, state_prev, decay_rate, rotation, log_step, in_re, in_im, read_re, read_im, skip_gain
):
    batch_rows = u_in.shape[0]
    groups = decay_rate.shape[0]
    grouped = u_in.astype(jnp.float32).reshape(batch_rows, groups, GROUP_CH)
    step_size = jnp.exp(log_step)[:, None]
    real_part = -decay_rate
    magnitude = jnp.exp(real_part * step_size)
    decay_re = magnitude * jnp.cos(rotation * step_size)
    decay_im = magnitude * jnp.sin(rotation * step_size)
    denominator = real_part * real_part + rotation * rotation
    lift_re = ((decay_re - 1.0) * real_part + decay_im * rotation) / denominator
    lift_im = (decay_im * real_part - (decay_re - 1.0) * rotation) / denominator
    map_re = lift_re[..., None] * in_re - lift_im[..., None] * in_im
    map_im = lift_re[..., None] * in_im + lift_im[..., None] * in_re
    drive_re = jnp.einsum("gph,bgh->bgp", map_re, grouped, precision=highest)
    drive_im = jnp.einsum("gph,bgh->bgp", map_im, grouped, precision=highest)
    old_re = state_prev[:, 0]
    old_im = state_prev[:, 1]
    new_re = decay_re * old_re - decay_im * old_im + drive_re
    new_im = decay_re * old_im + decay_im * old_re + drive_im
    output = (
        jnp.einsum("ghp,bgp->bgh", read_re, new_re, precision=highest)
        - jnp.einsum("ghp,bgp->bgh", read_im, new_im, precision=highest)
        + skip_gain * grouped
    )
    return (jax.nn.gelu(output.reshape(batch_rows, -1)), (new_re, new_im))


def fetch_kernel(spots, w_gate, w_up, gate_out, up_out, sems):
    width = gate_out.shape[1]
    copies = []
    for n in range(gate_out.shape[0]):
        start = pl.multiple_of(spots[n] * width, width)
        for m, (weights, out) in enumerate(((w_gate, gate_out), (w_up, up_out))):
            copy = pltpu.make_async_copy(weights.at[0, pl.ds(start, width)], out.at[n], sems.at[m, n])
            copy.start()
            copies.append(copy)
    for copy in copies:
        copy.wait()


def in_hbm(*arrays):
    return [pltpu.with_memory_space_constraint(a, pltpu.HBM) for a in arrays]


def fetch_weights(spots, w_gate, w_up, count, width):
    units = w_gate.shape[2]
    held = pltpu.VMEM((count, width, units), jnp.bfloat16)
    return pl.pallas_call(
        fetch_kernel,
        out_shape=[held, held],
        in_specs=[pl.BlockSpec(memory_space=pltpu.SMEM)] + [pl.BlockSpec(memory_space=pltpu.HBM)] * 2,
        out_specs=[pl.BlockSpec(memory_space=pltpu.VMEM)] * 2,
        scratch_shapes=[pltpu.SemaphoreType.DMA((2, count))],
        compiler_params=pltpu.CompilerParams(vmem_limit_bytes=2 * 2**20),
        cost_estimate=pl.CostEstimate(
            flops=0, bytes_accessed=4 * count * width * units, transcendentals=0
        ),
    )(spots, *in_hbm(w_gate, w_up))


def products_kernel(counts, full_width, streamed, first, last, *refs):
    refs = list(refs)
    spots = refs.pop(0)
    gains = refs.pop(0)
    pieces = [[refs.pop(0) for _ in range(n)] for n in counts]
    before = None if first else [refs.pop(0) for _ in range(3)]
    w_gate, w_up = refs.pop(0), refs.pop(0)
    outs = [refs.pop(0)] if last else [refs.pop(0) for _ in range(3)]
    scaled = refs.pop(0)
    gate_acc, up_acc = (refs.pop(0), refs.pop(0)) if last else outs[:2]
    width = scaled.shape[1]
    depth = width
    copies = []
    if streamed:
        gate_buf, up_buf, sems = refs
        depth = gate_buf.shape[1]
    steps = [(i, j) for i in range(len(counts)) for j in range(width // depth)]
    if streamed:
        for n, (i, j) in enumerate(steps):
            start = pl.multiple_of(spots[i] * width + j * depth, depth)
            for m, (weights, buf) in enumerate(((w_gate, gate_buf), (w_up, up_buf))):
                copy = pltpu.make_async_copy(
                    weights.at[0, pl.ds(start, depth)], buf.at[n], sems.at[m, n]
                )
                copy.start()
                copies.append(copy)
    else:
        gate_buf, up_buf = w_gate, w_up
    squares = 0.0 if first else before[2][...]
    for n, (i, j) in enumerate(steps):
        if j == 0:
            gain = gains[pl.ds(spots[i], 1), :]
            parts = []
            at = 0
            for group in pieces[i]:
                wide = group[...].astype(jnp.float32)
                parts.append(jnp.sum(wide * wide, axis=1, keepdims=True))
                scaled[at : at + group.shape[0], :] = (wide * gain).astype(jnp.bfloat16)
                at += group.shape[0]
            squares = squares + jnp.concatenate(parts, axis=0)
        left = scaled[:, j * depth : (j + 1) * depth]
        for m, (buf, acc) in enumerate(((gate_buf, gate_acc), (up_buf, up_acc))):
            if streamed:
                copies[2 * n + m].wait()
            product = jnp.dot(left, buf[n], preferred_element_type=jnp.float32)
            if n > 0:
                acc[...] += product
            elif first:
                acc[...] = product
            else:
                acc[...] = before[m][...] + product
    if last:
        scale = lax.rsqrt(squares / full_width + epsilon)
        outs[0][...] = (jax.nn.silu(gate_acc[...] * scale) * (up_acc[...] * scale)).astype(jnp.bfloat16)
    else:
        outs[2][...] = squares


def expert_products(spots, gains, pieces, before, w_gate, w_up, full_width, streamed, last):
    counts = tuple(len(groups) for groups in pieces)
    width = gains.shape[1]
    rows = sum(group.shape[0] for group in pieces[0])
    units = w_gate.shape[2]
    depth = min(width, 512)
    steps = len(pieces) * (width // depth)
    first = before is None
    whole = pl.BlockSpec(memory_space=pltpu.VMEM)
    inputs = [gains, *(group for groups in pieces for group in groups), *(() if first else before)]
    acc = jax.ShapeDtypeStruct((rows, units), jnp.float32)
    if last:
        out_shape = [jax.ShapeDtypeStruct((rows, units), jnp.bfloat16)]
    else:
        out_shape = [acc, acc, jax.ShapeDtypeStruct((rows, 1), jnp.float32)]
    scratch = [pltpu.VMEM((rows, width), jnp.bfloat16)]
    if last:
        scratch += [pltpu.VMEM((rows, units), jnp.float32)] * 2
    if streamed:
        scratch += [pltpu.VMEM((steps, depth, units), jnp.bfloat16)] * 2
        scratch += [pltpu.SemaphoreType.DMA((2, steps))]
        w_gate, w_up = in_hbm(w_gate, w_up)
    else:
        w_gate = pltpu.with_memory_space_constraint(w_gate, pltpu.VMEM)
        w_up = pltpu.with_memory_space_constraint(w_up, pltpu.VMEM)
    return pl.pallas_call(
        functools.partial(products_kernel, counts, full_width, streamed, first, last),
        out_shape=out_shape,
        in_specs=[pl.BlockSpec(memory_space=pltpu.SMEM)]
        + [whole] * len(inputs)
        + [pl.BlockSpec(memory_space=pltpu.HBM) if streamed else whole] * 2,
        out_specs=[whole] * len(out_shape),
        scratch_shapes=scratch,
        compiler_params=pltpu.CompilerParams(vmem_limit_bytes=(16 if streamed else 8) * 2**20),
        cost_estimate=pl.CostEstimate(
            flops=4 * rows * width * units * len(pieces),
            bytes_accessed=4 * width * units * len(pieces) if streamed else 0,
            transcendentals=0,
        ),
    )(spots, *inputs, w_gate, w_up)


def layer(
    residual,
    routes,
    route_weights,
    state_prev,
    mix_gain,
    ffn_gain,
    w_in,
    decay_rate,
    rotation,
    log_step,
    in_re,
    in_im,
    read_re,
    read_im,
    skip_gain,
    w_glu,
    w_out,
    w_gate,
    w_up,
    w_down,
):
    width = residual.shape[1]
    rows = residual.shape[0]
    tp_size = lax.axis_size("tp")
    ep_size = lax.axis_size("ep")
    chips = tp_size // 2
    full_width = width * tp_size
    place = lax.axis_index("tp")
    core = lax.bitwise_and(place, 1)
    chip = lax.shift_right_logical(place, 1)
    expert_here = lax.axis_index("ep")
    capacity = 2 * rows * TOPK // ep_size
    halves = ((0, ep_size // 2), (ep_size // 2, ep_size))
    f32 = jnp.float32
    bf16 = jnp.bfloat16

    def swap_core(value):
        return lax.ppermute(value, "tp", [(i, i ^ 1) for i in range(tp_size)])

    def swap_chip(value, step):
        return lax.ppermute(value, "tp", [(i, i ^ (2 * step)) for i in range(tp_size)])

    def swap_expert(value, step):
        return lax.ppermute(value, "ep", [(i, i ^ step) for i in range(ep_size)])

    def spot(step, same_core):
        return 2 * (chip ^ step) + (core if same_core else 1 - core)

    flat_routes = routes.reshape(-1)
    onehot = (flat_routes[:, None] == jnp.arange(ep_size, dtype=jnp.int32)).astype(jnp.int32)
    before = jnp.cumsum(onehot, axis=0) - onehot
    slot_index = jnp.sum(before * onehot, axis=1)
    relative = jnp.bitwise_xor(flat_routes, expert_here)
    destination = (relative * capacity + slot_index).reshape(rows, TOPK)
    matches = destination[:, :, None] == jnp.arange(ep_size * capacity, dtype=jnp.int32)
    dispatch_map = jnp.any(matches, axis=1).astype(bf16)
    gains = ffn_gain.reshape(tp_size, width)

    gathered = lax.all_gather(residual, "tp", axis=1, tiled=True).astype(f32)
    squares = jnp.mean(gathered * gathered, axis=1, keepdims=True)
    normed_mix = (gathered * lax.rsqrt(squares + epsilon) * mix_gain).astype(bf16)
    u_in = jnp.dot(normed_mix, w_in, preferred_element_type=f32).astype(bf16)
    mixer_act, state_next = state_mixer(
        u_in, state_prev, decay_rate, rotation, log_step, in_re, in_im, read_re, read_im, skip_gain
    )
    all_channels = lax.all_gather(mixer_act.astype(bf16), "tp", axis=1, tiled=True)
    glu_logit = jnp.dot(all_channels, w_glu, preferred_element_type=f32)
    mixed = lax.optimization_barrier((mixer_act * jax.nn.sigmoid(glu_logit)).astype(bf16))

    def branch_for(spot_of):
        part = lax.dynamic_slice_in_dim(w_out, spot_of * width, width, 1)
        return jnp.dot(mixed, part, preferred_element_type=f32)

    away = []
    for step in range(1, chips):
        theirs = swap_core(branch_for(spot(step, False)).astype(bf16))
        ours = branch_for(spot(step, True))
        away.append(swap_chip((ours + theirs.astype(f32)).astype(bf16), step))
    theirs = swap_core(branch_for(spot(0, False)).astype(bf16))
    branch = branch_for(spot(0, True)) + theirs.astype(f32)
    for piece in away:
        branch = branch + piece.astype(f32)
    after_mix = (residual.astype(f32) + branch).astype(bf16)

    outbound = lax.dot_general(
        dispatch_map, after_mix, (((0,), (0,)), ((), ())), preferred_element_type=f32
    ).astype(bf16)
    near_far = []
    for low, high in halves:
        blocks = [
            swap_expert(outbound[k * capacity : (k + 1) * capacity], k)
            if k
            else outbound[:capacity]
            for k in range(low, high)
        ]
        near_far.append(jnp.concatenate(blocks, axis=0))
    own = [(spot(0, True), near_far), (spot(0, False), [swap_core(h) for h in near_far])]
    held = []
    for same_core in (True, False):
        part = [spot(step, same_core) for step in range(1, chips)]
        part = jnp.stack(part).astype(jnp.int32)
        held.append(fetch_weights(part, w_gate, w_up, chips - 1, width))
    away = [[swap_chip(h, step) for h in near_far] for step in range(1, chips)]
    same = [(spot(step, True), away[step - 1]) for step in range(1, chips)]
    cross = [
        (spot(step, False), [swap_core(h) for h in away[step - 1]])
        for step in range(1, chips)
    ]
    sums = None
    for pieces, label in ((own, "own"), (same, "same"), (cross, "cross")):
        weights = (w_gate, w_up)
        if label != "own":
            weights = held[label == "cross"]
        spots = jnp.stack([p[0] for p in pieces]).astype(jnp.int32)
        sums = expert_products(
            spots,
            gains,
            [p[1] for p in pieces],
            sums,
            *weights,
            full_width,
            label == "own",
            label == "cross",
        )
    hidden = sums[0]

    def down_for(spot_of):
        part = lax.dynamic_slice_in_dim(w_down[0], spot_of * width, width, 1)
        return jnp.dot(hidden, part, preferred_element_type=f32)

    spans = [slice(low * capacity, high * capacity) for low, high in halves]
    away = []
    for step in range(1, chips):
        theirs = swap_core(down_for(spot(step, False)).astype(bf16))
        ours = (down_for(spot(step, True)) + theirs.astype(f32)).astype(bf16)
        ours = [ours[s] for s in spans]
        away.append([swap_chip(ours[i], step) for i in (1, 0)][::-1])
    theirs = swap_core(down_for(spot(0, False)).astype(bf16))
    home = down_for(spot(0, True)) + theirs.astype(f32)
    blocks = [None] * ep_size
    total = None
    for i in (1, 0):
        parts = [home[spans[i]]] + [piece[i] for piece in away]
        if total is not None:
            parts, total = lax.optimization_barrier((parts, total))
        total = sum(part.astype(f32) for part in parts).astype(bf16)
        for n, k in enumerate(range(*halves[i])):
            block = total[n * capacity : (n + 1) * capacity]
            blocks[k] = swap_expert(block, k) if k else block
    came_back = jnp.concatenate(blocks, axis=0)
    combined = 0.0
    for k in range(TOPK):
        picked = jnp.dot(matches[:, k].astype(bf16), came_back, preferred_element_type=f32)
        combined = combined + route_weights[:, k : k + 1] * picked
    layer_out = (after_mix.astype(f32) + combined).astype(bf16)
    state_next = jnp.stack(state_next, axis=1)
    return (layer_out, state_next)


def solution(mesh):
    return jax.shard_map(
        layer,
        mesh=mesh,
        in_specs=(
            P("ep", "tp"),
            P("ep", None),
            P("ep", None),
            P("ep", None, "tp", None),
            P(),
            P(),
            P(None, "tp"),
            P("tp", None),
            P("tp", None),
            P("tp"),
            P("tp", None, None),
            P("tp", None, None),
            P("tp", None, None),
            P("tp", None, None),
            P("tp", None),
            P(None, "tp"),
            P("tp", None),
            P("ep", None, "tp"),
            P("ep", None, "tp"),
            P("ep", "tp", None),
        ),
        out_specs=(P("ep", "tp"), P("ep", None, "tp", None)),
        check_vma=False,
    )
```
